32 devices in a mesh: sp: 4 (over z), tp: 4 (over y, x), dp: 2 (over core).
Axes of the slice: x: 2, y: 2, z: 4, core: 2. Of those that a mesh axis runs over, the one named last changes fastest.
Arguments:
- latent: bfloat16 [2048, 4, 2048], P(('sp', 'tp'), 'dp'), may hold values from -6 to 6
- context: bfloat16 [1024, 4, 2048], P('sp', 'dp'), may hold values from -6 to 6
- condition: bfloat16 [4, 2048], P('dp', 'sp'), may hold values from -6 to 6
- ctx_condition: bfloat16 [2048], P('sp'), may hold values from -6 to 6
- norm_gain: float32 [2048], replicated, may hold values from 0.1 to 1.9
- w_shift: bfloat16 [2048, 2048], P('sp', 'tp'), may hold values from -0.1875 to 0.1875
- w_scale: bfloat16 [2048, 2048], P('sp', 'tp'), may hold values from -0.1875 to 0.1875
- w_gate: bfloat16 [2048, 2048], P('sp', 'tp'), may hold values from -0.1875 to 0.1875
- w_query: bfloat16 [2048, 2048], P(None, 'tp'), may hold values from -0.125 to 0.125
- w_key: bfloat16 [2048, 512], P(None, 'tp'), may hold values from -6 to 6
- w_value: bfloat16 [2048, 512], P(None, 'tp'), may hold values from -0.125 to 0.125
- w_out: bfloat16 [2048, 2048], P('tp'), may hold values from -1 to 1
- sink: float32 [16], P('tp'), may hold values from 5 to 9
Outputs:
- mixed: bfloat16 [2048, 4, 2048], P(('sp', 'tp'), 'dp')
The draws below stay inside these ranges and needn't reach their ends.
All inputs are finite; a program needn't handle non-finite values.
Results may differ from the reference program's by a relative error of at most 0.015.
The reference program's roundings to bfloat16 on the way count: a program that leaves them out, or rounds other values in their place, can miss the bound.
Values may be sent and summed in bfloat16 or wider, within the bound.
A program may use at most 128 MiB of HBM per device.

```python
import jax
import jax.numpy as jnp
from jax import lax

D = 2048
HEADS = 16
KV_HEADS = 4
HEAD_DIM = 128
WINDOW = 128
GRID_W = 64
CTX = 1024
TOK_SP = 512
SEQ = 2048
SAMPLES = 4
N_SP = 4
N_TP = 4


def draw_w_key(key, part):
    matrix = jax.random.normal(key, (D, KV_HEADS * HEAD_DIM), jnp.float32) * D ** (-0.5)
    return jnp.clip(matrix, -6.0, 6.0).astype(jnp.bfloat16)


def block_levels(rng, shape, split, low, high):
    level = 1.0
    for dim, shards_of in split:
        draws = jax.random.uniform(jax.random.fold_in(jax.random.fold_in(rng, 6), dim), (shards_of,), jnp.float32, low / len(split), high / len(split))
        level = level * jnp.repeat(jnp.exp(draws), shape[dim] // shards_of).reshape((-1,) + (1,) * (len(shape) - 1 - dim))
    return level


def gaussian(key, dims, scale, reach, cuts=(), held_as=jnp.bfloat16):
    array = jax.random.normal(key, dims, jnp.float32) * scale
    if len(cuts) > 0:
        array = block_levels(key, dims, cuts, -0.22, 0.18) * array
    return jnp.clip(array, min=-reach, max=reach).astype(held_as)


def setup_inputs(seed: int = 0) -> dict:
    key_list = jax.random.split(jax.random.key(seed), 14)
    return {
        "latent": gaussian(key_list[0], (SEQ, SAMPLES, D), 1.0, 6.0, ((0, 16), (1, 2))),
        "context": gaussian(key_list[1], (CTX, SAMPLES, D), 1.0, 6.0, ((0, 4), (1, 2))),
        "condition": gaussian(key_list[2], (SAMPLES, D), 1.0, 6.0, ((0, 2), (1, 4))),
        "ctx_condition": gaussian(key_list[3], (D,), 1.0, 6.0, ((0, 4),)),
        "norm_gain": jnp.clip(1.0 + 0.18 * jax.random.normal(key_list[4], (D,), jnp.float32), 0.1, 1.9),
        "w_shift": gaussian(key_list[5], (D, D), (D // 2) ** -0.5, 0.1875, ((0, 4), (1, 4))),
        "w_scale": gaussian(key_list[6], (D, D), (D // 2) ** -0.5, 0.1875, ((0, 4), (1, 4))),
        "w_gate": gaussian(key_list[7], (D, D), (D // 2) ** -0.5, 0.1875, ((0, 4), (1, 4))),
        "w_query": gaussian(key_list[8], (D, HEADS * HEAD_DIM), D ** -0.5, 0.125, ((1, 4),)),
        "w_key": draw_w_key(jax.random.fold_in(key_list[13], 71), 0),
        "w_value": gaussian(key_list[10], (D, KV_HEADS * HEAD_DIM), D ** -0.5, 0.125, ((1, 4),)),
        "w_out": gaussian(key_list[11], (HEADS * HEAD_DIM, D), (HEAD_DIM // 4) ** -0.5, 1.0, ((0, 4),)),
        "sink": jnp.clip(5.0 + 4.0 * jax.random.uniform(key_list[12], (HEADS,), jnp.float32) ** block_levels(key_list[12], (HEADS,), ((0, 4),), -0.2, 0.2), 5.0, 9.0),
    }


EPSILON = 1e-06
NEGATIVE = -1e+30

def normed(values, gain):
    floats = values.astype(jnp.float32)
    return floats * lax.rsqrt(lax.optimization_barrier(jnp.mean(floats * floats, axis=-1, keepdims=True)) + EPSILON) * gain

def rotate(tensor, position):
    quarter = HEAD_DIM // 4
    freqs = 10000.0 ** (-jnp.arange(quarter, dtype=jnp.float32) / quarter)
    row_pos = (position // GRID_W).astype(jnp.float32)
    col_pos = (position % GRID_W).astype(jnp.float32)
    angle = jnp.stack([row_pos[:, None] * freqs, col_pos[:, None] * freqs], axis=1)
    cosine = jnp.cos(angle)[:, None, None]
    sine = jnp.sin(angle)[:, None, None]
    pieces = tensor.reshape(tensor.shape[:-1] + (2, 2, quarter))
    first = pieces[..., 0, :]
    second = pieces[..., 1, :]
    turned = jnp.stack([first * cosine - second * sine, second * cosine + first * sine], axis=-2)
    return turned.reshape(tensor.shape)

def attend_block(queries, keys, values, allowed, ctx_keys, ctx_values, sink_logit):
    q_rows, batch, heads_n, width = queries.shape
    kv_heads = keys.shape[2]
    grouped = queries.reshape(q_rows, batch, kv_heads, heads_n // kv_heads, width).astype(jnp.float32)
    factor = width ** (-0.5)
    local_scores = jnp.einsum('qbkgd,jbkd->bkgqj', grouped, keys.astype(jnp.float32)) * factor
    local_scores = jnp.where(allowed, local_scores, NEGATIVE)
    ctx_scores = jnp.einsum('qbkgd,jbkd->bkgqj', grouped, ctx_keys.astype(jnp.float32)) * factor
    sink_scores = sink_logit.astype(jnp.float32).reshape(kv_heads, heads_n // kv_heads)[None, :, :, None, None]
    top = jnp.maximum(jnp.maximum(lax.optimization_barrier(jnp.max(local_scores, axis=-1, keepdims=True)), lax.optimization_barrier(jnp.max(ctx_scores, axis=-1, keepdims=True))), sink_scores)
    local_exp = jnp.exp(local_scores - top)
    ctx_exp = jnp.exp(ctx_scores - top)
    total = lax.optimization_barrier(jnp.sum(local_exp, axis=-1, keepdims=True)) + lax.optimization_barrier(jnp.sum(ctx_exp, axis=-1, keepdims=True)) + jnp.exp(sink_scores - top)
    local_weights = (local_exp / total).astype(jnp.bfloat16)
    ctx_weights = (ctx_exp / total).astype(jnp.bfloat16)
    result = jnp.einsum('bkgqj,jbkd->qbkgd', local_weights.astype(jnp.float32), values.astype(jnp.float32))
    result = result + jnp.einsum('bkgqj,jbkd->qbkgd', ctx_weights.astype(jnp.float32), ctx_values.astype(jnp.float32))
    return result.astype(jnp.bfloat16).reshape(q_rows, batch, heads_n * width)

def reference(latent, context, condition, ctx_condition, norm_gain, w_shift, w_scale, w_gate, w_query, w_key, w_value, w_out, sink):
    act = jax.nn.silu(condition.astype(jnp.float32)).astype(jnp.bfloat16)
    ctx_act = jax.nn.silu(ctx_condition.astype(jnp.float32)).astype(jnp.bfloat16)
    both = jnp.concatenate([act, ctx_act[None]], axis=0)
    shift_all = jnp.dot(both, w_shift, preferred_element_type=jnp.float32)
    scale_all = jnp.dot(both, w_scale, preferred_element_type=jnp.float32)
    gate = jnp.dot(act, w_gate, preferred_element_type=jnp.float32)
    samples_n = latent.shape[1]
    hidden = (normed(latent, norm_gain) * (1.0 + scale_all[None, :samples_n]) + shift_all[None, :samples_n]).astype(jnp.bfloat16)
    ctx_hidden = (normed(context, norm_gain) * (1.0 + scale_all[samples_n]) + shift_all[samples_n]).astype(jnp.bfloat16)
    seq_len = latent.shape[0]
    position = jnp.arange(seq_len, dtype=jnp.int32)
    queries = jnp.dot(hidden, w_query, preferred_element_type=jnp.float32).reshape(seq_len, samples_n, HEADS, HEAD_DIM)
    queries = rotate(queries, position).astype(jnp.bfloat16)
    keys = jnp.dot(hidden, w_key, preferred_element_type=jnp.float32).reshape(seq_len, samples_n, KV_HEADS, HEAD_DIM)
    keys = rotate(keys, position).astype(jnp.bfloat16)
    values = jnp.dot(hidden, w_value, preferred_element_type=jnp.float32).astype(jnp.bfloat16).reshape(seq_len, samples_n, KV_HEADS, HEAD_DIM)
    ctx_keys = jnp.dot(ctx_hidden, w_key, preferred_element_type=jnp.float32).astype(jnp.bfloat16).reshape(CTX, samples_n, KV_HEADS, HEAD_DIM)
    ctx_values = jnp.dot(ctx_hidden, w_value, preferred_element_type=jnp.float32).astype(jnp.bfloat16).reshape(CTX, samples_n, KV_HEADS, HEAD_DIM)
    padding = ((WINDOW, WINDOW), (0, 0), (0, 0), (0, 0))
    keys_pad = jnp.pad(keys, padding)
    values_pad = jnp.pad(values, padding)
    span = TOK_SP + 2 * WINDOW

    def one_block(block):
        start = (block * TOK_SP).astype(jnp.int32)
        block_q = lax.dynamic_slice_in_dim(queries, start, TOK_SP, 0)
        block_k = lax.dynamic_slice_in_dim(keys_pad, start, span, 0)
        block_v = lax.dynamic_slice_in_dim(values_pad, start, span, 0)
        q_pos = start + jnp.arange(TOK_SP, dtype=jnp.int32)
        k_pos = start - WINDOW + jnp.arange(span, dtype=jnp.int32)
        allowed = (jnp.abs(k_pos[None, :] - q_pos[:, None]) <= WINDOW) & (k_pos >= 0)[None, :] & (k_pos < seq_len)[None, :]
        return attend_block(block_q, block_k, block_v, allowed, ctx_keys, ctx_values, sink)
    attn = lax.map(one_block, jnp.arange(N_SP, dtype=jnp.int32)).reshape(seq_len, samples_n, HEADS * HEAD_DIM)
    group_width = HEADS * HEAD_DIM // N_TP
    branch = jnp.zeros((seq_len, samples_n, D), jnp.float32)
    for group in range(N_TP):
        part = jnp.dot(attn[..., group * group_width:(group + 1) * group_width], w_out[group * group_width:(group + 1) * group_width], preferred_element_type=jnp.float32)
        branch = branch + part.astype(jnp.bfloat16).astype(jnp.float32)
    return (latent.astype(jnp.float32) + gate[None] * branch).astype(jnp.bfloat16)
```

```python
import functools
import math

import jax
import jax.numpy as jnp
from jax import lax
from jax.experimental import pallas as pl
from jax.experimental.pallas import tpu as pltpu
from jax.sharding import PartitionSpec as P

HEAD_DIM = 128
WINDOW = 128
GRID_W = 64
EPSILON = 1e-06
NEGATIVE = -1e30
MESH = pl.DeviceIdType.MESH
F32 = jnp.float32
BF16 = jnp.bfloat16
LOG2E = math.log2(math.e)
CHUNK = 16
SENDS = ((3, 0), (3, 1), (1, 0), (2, 1), (2, 0), (1, 1), (0, 0), (0, 1))
TARGETS = (1, 2, 1, 2, 2, 1)


def kernel(
    n_sp,
    lat_hbm,
    ctx_hbm,
    cond_ref,
    cctx_ref,
    gain_ref,
    wsh_hbm,
    wsc_hbm,
    wga_hbm,
    wq_hbm,
    wk_hbm,
    wv_hbm,
    wo_hbm,
    sink_ref,
    cos_ref,
    sin_ref,
    out_ref,
    lat_all,
    ctx_v,
    wmod,
    wqkv,
    wo,
    act_s,
    mod_p,
    mod_all,
    mod_a,
    mod_b,
    mod_g,
    hbuf,
    qbuf,
    kvbuf,
    ckv,
    abuf,
    psend,
    rs,

    loc_sem,
    modp_s,
    modp_r,
    moda_s,
    moda_r,
    lat_s,
    lat_r,
    ctx_s,
    ctx_r,
    halo_s,
    halo_r,
    rs_s,
    rs_r,
):
    samples, rows, width = lat_hbm.shape
    n_tp = mod_all.shape[0]
    wid = wmod.shape[2]
    qw = wq_hbm.shape[1]
    kw = wk_hbm.shape[1]
    heads = qw // HEAD_DIM
    lc = ctx_hbm.shape[1]
    block = rows * n_tp
    sp = lax.axis_index("sp")
    tp = lax.axis_index("tp")
    tx, ty = tp % 2, tp // 2
    peer = {1: 2 * ty + 1 - tx, 2: 2 * (1 - ty) + tx, 3: 3 - tp}

    def sp_peer(o):
        return lax.rem(sp + o, n_sp)

    loads = [
        pltpu.make_async_copy(wsh_hbm, wmod.at[0], loc_sem.at[0]),
        pltpu.make_async_copy(wsc_hbm, wmod.at[1], loc_sem.at[1]),
        pltpu.make_async_copy(wga_hbm, wmod.at[2], loc_sem.at[2]),
        pltpu.make_async_copy(ctx_hbm, ctx_v, loc_sem.at[3]),
        pltpu.make_async_copy(wk_hbm, wqkv.at[:, pl.ds(qw, kw)], loc_sem.at[4]),
        pltpu.make_async_copy(wv_hbm, wqkv.at[:, pl.ds(qw + kw, kw)], loc_sem.at[5]),
        pltpu.make_async_copy(lat_hbm, lat_all.at[0], loc_sem.at[6]),
        pltpu.make_async_copy(wq_hbm, wqkv.at[:, pl.ds(0, qw)], loc_sem.at[7]),
        pltpu.make_async_copy(wo_hbm, wo, loc_sem.at[8]),
    ]
    for load in loads:
        load.start()

    barrier = pltpu.get_barrier_semaphore()
    for o in range(1, n_sp):
        pl.semaphore_signal(barrier, inc=1, device_id={"sp": sp_peer(o)}, device_id_type=MESH)
    for k in (1, 2, 3):
        pl.semaphore_signal(barrier, inc=1, device_id={"tp": peer[k]}, device_id_type=MESH)
    pl.semaphore_wait(barrier, n_sp - 1 + n_tp - 1)

    def remote(src, dst, ssem, rsem, dev):
        return pltpu.make_async_remote_copy(
            src_ref=src, dst_ref=dst, send_sem=ssem, recv_sem=rsem, device_id=dev, device_id_type=MESH
        )

    act_s[...] = jnp.zeros_like(act_s)
    cv = cond_ref[...].astype(F32)
    act_s[0:samples, :] = cv / (1.0 + jnp.exp(-cv))
    cc = cctx_ref[...].astype(F32)
    act_s[samples : samples + 1, :] = cc / (1.0 + jnp.exp(-cc))
    both = act_s[...].astype(BF16)
    for m in range(3):
        loads[m].wait()
        mod_p[0, :, m * wid : (m + 1) * wid] = jnp.dot(both, wmod[m], preferred_element_type=F32)
    mod_copies = [
        remote(mod_p.at[0], mod_p.at[o], modp_s.at[o], modp_r.at[o], {"sp": sp_peer(o)})
        for o in range(1, n_sp)
    ]
    for copy in mod_copies:
        copy.start()

    def lat_copy(k, s, relay):
        if not relay:
            return remote(
                lat_hbm.at[s], lat_all.at[k, s], lat_s.at[k, s], lat_r.at[k, s], {"tp": peer[k]}
            )
        via, to = (1, 2) if s == 0 else (2, 1)
        return remote(
            lat_all.at[via, s], lat_all.at[3, s], lat_s.at[3, s], lat_r.at[3, s], {"tp": peer[to]}
        )

    for k, s in ((1, 0), (2, 1), (1, 1), (2, 0)):
        lat_copy(k, s, False).start()

    for copy in mod_copies:
        copy.wait_recv()
    total = mod_p[0]
    for o in range(1, n_sp):
        total = total + mod_p[o]
    mod_all[tp] = total
    all_copies = [
        remote(mod_all.at[tp], mod_all.at[tp], moda_s.at[k], moda_r.at[k], {"tp": peer[k]})
        for k in (1, 2, 3)
    ]
    for copy in all_copies:
        copy.start()
    for k in (1, 2, 3):
        remote(
            mod_all.at[peer[k]], mod_all.at[peer[k]], moda_s.at[k], moda_r.at[k], {"tp": peer[k]}
        ).wait_recv()
    for t in range(n_tp):
        cols = slice(t * wid, (t + 1) * wid)
        mod_b[:, cols] = mod_all[t, :, 0:wid]
        mod_a[:, cols] = (1.0 + mod_all[t, :, wid : 2 * wid]) * gain_ref[:, cols]
        mod_g[:, cols] = mod_all[t, :, 2 * wid : 3 * wid]

    def norm_rows(src, mod_row, base, count):
        a_row = mod_a[pl.ds(mod_row, 1), :]
        b_row = mod_b[pl.ds(mod_row, 1), :]

        @pl.loop(0, count // CHUNK)
        def _(c):
            at = pl.multiple_of(c * CHUNK, CHUNK)
            x = src[pl.ds(at, CHUNK), :].astype(F32)
            inv = lax.rsqrt(jnp.mean(x * x, axis=-1, keepdims=True) + EPSILON)
            hbuf[pl.ds(base + at, CHUNK), :] = (x * inv * a_row + b_row).astype(BF16)

    for i in (3, 4, 5):
        loads[i].wait()
    ctx_at = pl.multiple_of(sp * lc, lc)

    @pl.loop(0, samples)
    def _(s):
        norm_rows(ctx_v.at[s], samples, 0, lc)
        ckv[s, pl.ds(ctx_at, lc), :] = jnp.dot(
            hbuf[0:lc, :], wqkv[:, qw : qw + 2 * kw], preferred_element_type=F32
        ).astype(BF16)

    mine = ckv.at[:, pl.ds(ctx_at, lc), :]
    ctx_copies = [
        remote(mine, mine, ctx_s.at[o], ctx_r.at[o], {"sp": sp_peer(o)}) for o in range(1, n_sp)
    ]
    for copy in ctx_copies:
        copy.start()

    for s in (0, 1):
        lat_copy(1 if s == 0 else 2, s, False).wait_recv()
        lat_copy(3, s, True).start()

    loads[6].wait()
    loads[7].wait()
    lane = lax.broadcasted_iota(jnp.int32, (rows, HEAD_DIM), 1)
    low = lane % (HEAD_DIM // 2) < HEAD_DIM // 4

    def turn(u, cos, sin):
        other = jnp.where(
            low, pltpu.roll(u, HEAD_DIM - HEAD_DIM // 4, 1), pltpu.roll(u, HEAD_DIM // 4, 1)
        )
        return u * cos + other * sin

    @pl.loop(0, n_tp)
    def _(k):
        @pl.when(k == 1)
        def _():
            lat_copy(1, 1, False).wait_recv()

        @pl.when(k == 2)
        def _():
            lat_copy(2, 0, False).wait_recv()

        @pl.when(k == 3)
        def _():
            lat_copy(3, 0, True).wait_recv()
            lat_copy(3, 1, True).wait_recv()

        kx, ky = k % 2, k // 2
        bx = tx + kx - 2 * tx * kx
        by = ty + ky - 2 * ty * ky
        b = 2 * by + bx
        for s in range(samples):
            norm_rows(lat_all.at[k, s], s, s * rows, rows)
        at = pl.multiple_of(b * rows, rows)
        cos = cos_ref[pl.ds(at, rows), :]
        sin = sin_ref[pl.ds(at, rows), :]
        for c in range(heads // 2 + 1):
            prod = jnp.dot(
                hbuf[...], wqkv[:, c * 2 * HEAD_DIM : (c + 1) * 2 * HEAD_DIM], preferred_element_type=F32
            )
            for s in range(samples):
                part = prod[s * rows : (s + 1) * rows]
                first = turn(part[:, :HEAD_DIM], cos, sin).astype(BF16)
                if c < heads // 2:
                    second = turn(part[:, HEAD_DIM:], cos, sin).astype(BF16)
                    qbuf[s, b, 2 * c * rows : (2 * c + 1) * rows, :] = first
                    qbuf[s, b, (2 * c + 1) * rows : (2 * c + 2) * rows, :] = second
                else:
                    kvbuf[s, pl.ds(WINDOW + at, rows), 0:HEAD_DIM] = first
                    kvbuf[s, pl.ds(WINDOW + at, rows), HEAD_DIM:] = part[:, HEAD_DIM:].astype(BF16)

    halo_up = remote(
        kvbuf.at[:, pl.ds(block, WINDOW), :],
        kvbuf.at[:, pl.ds(0, WINDOW), :],
        halo_s.at[0],
        halo_r.at[0],
        {"sp": sp_peer(1)},
    )
    halo_down = remote(
        kvbuf.at[:, pl.ds(WINDOW, WINDOW), :],
        kvbuf.at[:, pl.ds(WINDOW + block, WINDOW), :],
        halo_s.at[1],
        halo_r.at[1],
        {"sp": sp_peer(n_sp - 1)},
    )
    halo_up.start()
    halo_down.start()
    loads[8].wait()
    for o in range(1, n_sp):
        got = ckv.at[:, pl.ds(pl.multiple_of(sp_peer(n_sp - o) * lc, lc), lc), :]
        remote(got, got, ctx_s.at[o], ctx_r.at[o], {"sp": sp_peer(o)}).wait_recv()
    halo_up.wait()
    halo_down.wait()

    scale = HEAD_DIM ** (-0.5) * LOG2E
    seq = block * n_sp
    nums = (((1,), (1,)), ((), ()))

    def rs_copy(i):
        return remote(
            psend.at[i], rs.at[i], rs_s.at[i], rs_r.at[i], {"tp": peer[TARGETS[i]]}
        )

    def pick(i, which):
        value = SENDS[-1][which]
        for j in range(len(SENDS) - 1):
            value = jnp.where(i == j, SENDS[j][which], value)
        return value

    span = 3 * WINDOW
    pair = 2 * rows
    row_id = lax.broadcasted_iota(jnp.int32, (pair, 1), 0)

    @pl.loop(0, 8)
    def _(i):
        k = pick(i, 0)
        s = pick(i, 1)
        kx, ky = k % 2, k // 2
        b = 2 * (ty + ky - 2 * ty * ky) + tx + kx - 2 * tx * kx
        at = pl.multiple_of(b * rows, rows)
        kc = ckv[s, :, 0:HEAD_DIM]
        vc = ckv[s, :, HEAD_DIM:]
        kl = kvbuf[s, pl.ds(at, span), 0:HEAD_DIM]
        vl = kvbuf[s, pl.ds(at, span), HEAD_DIM:]
        key = lax.broadcasted_iota(jnp.int32, (pair, span), 1)
        query = lax.broadcasted_iota(jnp.int32, (pair, span), 0) % rows
        pos = key + (sp * block + b * rows - WINDOW)
        allowed = (key >= query) & (key <= query + 2 * WINDOW) & (pos >= 0) & (pos < seq)
        for c in range(heads // 2):
            q = qbuf[s, b, c * pair : (c + 1) * pair, :]
            sc = lax.dot_general(q, kc, nums, preferred_element_type=F32)
            sl = lax.dot_general(q, kl, nums, preferred_element_type=F32)
            sl = jnp.where(allowed, sl, NEGATIVE)
            sink2 = jnp.where(row_id < rows, sink_ref[0, 2 * c], sink_ref[0, 2 * c + 1]) * LOG2E
            top = jnp.maximum(
                jnp.max(sc, axis=-1, keepdims=True), jnp.max(sl, axis=-1, keepdims=True)
            )
            top = jnp.maximum(top * scale, sink2)
            ec = jnp.exp2(sc * scale - top)
            el = jnp.exp2(sl * scale - top)
            total = (
                jnp.sum(ec, axis=-1, keepdims=True)
                + jnp.sum(el, axis=-1, keepdims=True)
                + jnp.exp2(sink2 - top)
            )
            o = jnp.dot(ec.astype(BF16), vc, preferred_element_type=F32)
            o = o + jnp.dot(el.astype(BF16), vl, preferred_element_type=F32)
            o = (o / total).astype(BF16)
            abuf[:, 2 * c * HEAD_DIM : (2 * c + 1) * HEAD_DIM] = o[:rows]
            abuf[:, (2 * c + 1) * HEAD_DIM : (2 * c + 2) * HEAD_DIM] = o[rows:]
        for n in range(n_tp):
            cols = slice(n * wid, (n + 1) * wid)
            psend[i, :, cols] = jnp.dot(
                abuf[...], wo[:, cols], preferred_element_type=F32
            ).astype(BF16)

        for j in range(4):

            @pl.when(i == j)
            def _(j=j):
                rs_copy(j).start()

        for j in (4, 5):

            @pl.when(i == j)
            def _(j=j):
                rs_copy(j - 4).wait_recv()

                @pl.loop(0, rows // CHUNK)
                def _(r):
                    part = pl.ds(pl.multiple_of(r * CHUNK, CHUNK), CHUNK)
                    psend[j, part, :] = (
                        psend[j, part, :].astype(F32) + rs[j - 4, part, :].astype(F32)
                    ).astype(BF16)

                rs_copy(j).start()

    for s in range(2):
        rs_copy(2 + s).wait_recv()
        rs_copy(4 + s).wait_recv()
        g_row = mod_g[s : s + 1, :]

        @pl.loop(0, rows // CHUNK)
        def _(r, s=s, g_row=g_row):
            part = pl.ds(pl.multiple_of(r * CHUNK, CHUNK), CHUNK)
            branch = (
                psend[6 + s, part, :].astype(F32)
                + rs[2 + s, part, :].astype(F32)
                + rs[4 + s, part, :].astype(F32)
            )
            out_ref[s, part, :] = (
                lat_all[0, s, part, :].astype(F32) + g_row * branch
            ).astype(BF16)

    for copy in mod_copies + all_copies + ctx_copies:
        copy.wait_send()
    for k, s in ((1, 0), (2, 1), (1, 1), (2, 0)):
        lat_copy(k, s, False).wait_send()
    for s in (0, 1):
        lat_copy(3, s, True).wait_send()
    for i in range(6):
        rs_copy(i).wait_send()


def local(
    n_sp,
    n_tp,
    latent,
    context,
    condition,
    ctx_condition,
    norm_gain,
    w_shift,
    w_scale,
    w_gate,
    w_query,
    w_key,
    w_value,
    w_out,
    sink,
):
    rows, samples, width = latent.shape
    lc = context.shape[0]
    wid = w_shift.shape[1]
    depth = w_shift.shape[0]
    qw, kw = w_query.shape[1], w_key.shape[1]
    heads = qw // HEAD_DIM
    block = rows * n_tp
    assert n_tp == 4 and samples == 2 and kw == HEAD_DIM and rows == WINDOW and heads % 2 == 0
    position = lax.axis_index("sp") * block + jnp.arange(block, dtype=jnp.int32)
    quarter = HEAD_DIM // 4
    lane = jnp.arange(HEAD_DIM, dtype=jnp.int32)
    freqs = 10000.0 ** (-(lane % quarter).astype(F32) / quarter)
    grid_pos = jnp.where(
        (lane < HEAD_DIM // 2)[None, :], (position // GRID_W)[:, None], (position % GRID_W)[:, None]
    ).astype(F32)
    angle = grid_pos * freqs[None, :]
    sign = jnp.where(lane % (2 * quarter) < quarter, -1.0, 1.0).astype(F32)
    cos = jnp.cos(angle)
    sin = jnp.sin(angle) * sign[None, :]
    hbm = pl.BlockSpec(memory_space=pl.ANY)
    vmem = pl.BlockSpec(memory_space=pltpu.VMEM)
    smem = pl.BlockSpec(memory_space=pltpu.SMEM)
    dma = pltpu.SemaphoreType.DMA
    mixed = pl.pallas_call(
        functools.partial(kernel, n_sp),
        out_shape=jax.ShapeDtypeStruct((samples, rows, width), BF16),
        in_specs=[hbm, hbm, vmem, vmem, vmem, hbm, hbm, hbm, hbm, hbm, hbm, hbm, smem, vmem, vmem],
        out_specs=vmem,
        scratch_shapes=[
            pltpu.VMEM((n_tp, samples, rows, width), BF16),
            pltpu.VMEM((samples, lc, width), BF16),
            pltpu.VMEM((3, depth, wid), BF16),
            pltpu.VMEM((width, qw + 2 * kw), BF16),
            pltpu.VMEM((qw, width), BF16),
            pltpu.VMEM((8, depth), F32),
            pltpu.VMEM((n_sp, 8, 3 * wid), F32),
            pltpu.VMEM((n_tp, 8, 3 * wid), F32),
            pltpu.VMEM((8, width), F32),
            pltpu.VMEM((8, width), F32),
            pltpu.VMEM((8, width), F32),
            pltpu.VMEM((max(samples * rows, lc), width), BF16),
            pltpu.VMEM((samples, n_tp, heads * rows, HEAD_DIM), BF16),
            pltpu.VMEM((samples, block + 2 * WINDOW, 2 * kw), BF16),
            pltpu.VMEM((samples, lc * n_sp, 2 * kw), BF16),
            pltpu.VMEM((rows, qw), BF16),
            pltpu.VMEM((8, rows, width), BF16),
            pltpu.VMEM((6, rows, width), BF16),
            dma((9,)),
            dma((n_sp,)),
            dma((n_sp,)),
            dma((n_tp,)),
            dma((n_tp,)),
            dma((n_tp, 2)),
            dma((n_tp, 2)),
            dma((n_sp,)),
            dma((n_sp,)),
            dma((2,)),
            dma((2,)),
            dma((6,)),
            dma((6,)),
        ],
        compiler_params=pltpu.CompilerParams(
            collective_id=0, has_side_effects=True, vmem_limit_bytes=60 * 1024 * 1024
        ),
        name="step",
    )(
        latent.transpose(1, 0, 2),
        context.transpose(1, 0, 2),
        condition,
        ctx_condition[None],
        norm_gain[None],
        w_shift,
        w_scale,
        w_gate,
        w_query,
        w_key,
        w_value,
        w_out,
        sink[None],
        cos,
        sin,
    )
    return mixed.transpose(1, 0, 2)


def solution(mesh):
    return jax.shard_map(
        functools.partial(local, mesh.shape["sp"], mesh.shape["tp"]),
        mesh=mesh,
        in_specs=(
            P(("sp", "tp"), "dp", None),
            P("sp", "dp", None),
            P("dp", "sp"),
            P("sp"),
            P(),
            P("sp", "tp"),
            P("sp", "tp"),
            P("sp", "tp"),
            P(None, "tp"),
            P(None, "tp"),
            P(None, "tp"),
            P("tp", None),
            P("tp"),
        ),
        out_specs=P(("sp", "tp"), "dp", None),
        check_vma=False,
    )
```

```python
import functools
import math

import jax
import jax.numpy as jnp
from jax import lax
from jax.experimental import pallas as pl
from jax.experimental.pallas import tpu as pltpu
from jax.sharding import PartitionSpec as P

HEAD_DIM = 128
WINDOW = 128
GRID_W = 64
EPSILON = 1e-06
NEGATIVE = -1e30
MESH = pl.DeviceIdType.MESH
F32 = jnp.float32
BF16 = jnp.bfloat16
LOG2E = math.log2(math.e)
CHUNK = 16
SENDS = ((3, 0), (3, 1), (1, 0), (2, 1), (2, 0), (1, 1), (0, 0), (0, 1))
TARGETS = (1, 2, 1, 2, 2, 1)


def kernel(
    n_sp,
    lat_hbm,
    ctx_hbm,
    cond_ref,
    cctx_ref,
    gain_ref,
    wsh_hbm,
    wsc_hbm,
    wga_hbm,
    wq_hbm,
    wk_hbm,
    wv_hbm,
    wo_hbm,
    sink_ref,
    row_ref,
    col_ref,
    out_ref,
    lat_all,
    ctx_v,
    wmod,
    wqkv,
    wo,
    act_s,
    mod_p,
    mod_all,
    mod_a,
    mod_b,
    mod_g,
    hbuf,
    qbuf,
    kvbuf,
    ckv,
    abuf,
    cos_ref,
    sin_ref,
    psend,
    rs,

    loc_sem,
    modp_s,
    modp_r,
    moda_s,
    moda_r,
    lat_s,
    lat_r,
    early_s,
    early_r,
    ctx_s,
    ctx_r,
    halo_s,
    halo_r,
    rs_s,
    rs_r,
):
    samples, rows, width = lat_hbm.shape
    n_tp = mod_all.shape[0]
    wid = wmod.shape[2]
    qw = wq_hbm.shape[1]
    kw = wk_hbm.shape[1]
    heads = qw // HEAD_DIM
    lc = ctx_hbm.shape[1]
    block = rows * n_tp
    sp = lax.axis_index("sp")
    tp = lax.axis_index("tp")
    tx, ty = tp % 2, tp // 2
    peer = {1: 2 * ty + 1 - tx, 2: 2 * (1 - ty) + tx, 3: 3 - tp}

    def sp_peer(o):
        return lax.rem(sp + o, n_sp)

    loads = [
        pltpu.make_async_copy(wsh_hbm, wmod.at[0], loc_sem.at[0]),
        pltpu.make_async_copy(wsc_hbm, wmod.at[1], loc_sem.at[1]),
        pltpu.make_async_copy(wga_hbm, wmod.at[2], loc_sem.at[2]),
        pltpu.make_async_copy(ctx_hbm, ctx_v, loc_sem.at[3]),
        pltpu.make_async_copy(wk_hbm, wqkv.at[:, pl.ds(qw, kw)], loc_sem.at[4]),
        pltpu.make_async_copy(wv_hbm, wqkv.at[:, pl.ds(qw + kw, kw)], loc_sem.at[5]),
        pltpu.make_async_copy(lat_hbm, lat_all.at[0], loc_sem.at[6]),
        pltpu.make_async_copy(wq_hbm, wqkv.at[:, pl.ds(0, qw)], loc_sem.at[7]),
        pltpu.make_async_copy(wo_hbm, wo, loc_sem.at[8]),
    ]
    for load in loads:
        load.start()

    barrier = pltpu.get_barrier_semaphore()
    for o in range(1, n_sp):
        pl.semaphore_signal(barrier, inc=1, device_id={"sp": sp_peer(o)}, device_id_type=MESH)
    for k in (1, 2, 3):
        pl.semaphore_signal(barrier, inc=1, device_id={"tp": peer[k]}, device_id_type=MESH)
    pl.semaphore_wait(barrier, n_sp - 1 + n_tp - 1)

    def remote(src, dst, ssem, rsem, dev):
        return pltpu.make_async_remote_copy(
            src_ref=src, dst_ref=dst, send_sem=ssem, recv_sem=rsem, device_id=dev, device_id_type=MESH
        )

    act_s[...] = jnp.zeros_like(act_s)
    cv = cond_ref[...].astype(F32)
    act_s[0:samples, :] = cv / (1.0 + jnp.exp(-cv))
    cc = cctx_ref[...].astype(F32).reshape(1, -1)
    act_s[samples : samples + 1, :] = cc / (1.0 + jnp.exp(-cc))
    both = act_s[...].astype(BF16)
    for m in range(3):
        loads[m].wait()
        mod_p[0, :, m * wid : (m + 1) * wid] = jnp.dot(both, wmod[m], preferred_element_type=F32)
    mod_copies = [
        remote(mod_p.at[0], mod_p.at[o], modp_s.at[o], modp_r.at[o], {"sp": sp_peer(o)})
        for o in range(1, n_sp)
    ]
    for copy in mod_copies:
        copy.start()

    def lat_copy(k, s, relay):
        if not relay:
            return remote(
                lat_hbm.at[s], lat_all.at[k, s], lat_s.at[k, s], lat_r.at[k, s], {"tp": peer[k]}
            )
        via, to = (1, 2) if s == 0 else (2, 1)
        return remote(
            lat_all.at[via, s], lat_all.at[3, s], lat_s.at[3, s], lat_r.at[3, s], {"tp": peer[to]}
        )

    half = rows // 2

    def lat_part(k, s, p):
        part = pl.ds(p * half, half)
        return remote(
            lat_hbm.at[s, part], lat_all.at[k, s, part], early_s.at[k, p], early_r.at[k, p], {"tp": peer[k]}
        )

    lat_part(1, 0, 0).start()
    lat_part(2, 1, 0).start()

    for which, table in ((0, cos_ref), (1, sin_ref)):
        left = lax.broadcasted_iota(jnp.int32, (GRID_W, HEAD_DIM), 1) < HEAD_DIM // 2
        for r in range(block // GRID_W):
            table[r * GRID_W : (r + 1) * GRID_W, :] = jnp.where(
                left, row_ref[which, r : r + 1, :], col_ref[which]
            )

    for copy in mod_copies:
        copy.wait_recv()
    total = mod_p[0]
    for o in range(1, n_sp):
        total = total + mod_p[o]
    mod_all[tp] = total
    all_copies = [
        remote(mod_all.at[tp], mod_all.at[tp], moda_s.at[k], moda_r.at[k], {"tp": peer[k]})
        for k in (1, 2, 3)
    ]
    for copy in all_copies:
        copy.start()
    lat_part(1, 0, 1).start()
    lat_part(2, 1, 1).start()
    lat_copy(1, 1, False).start()
    lat_copy(2, 0, False).start()
    for k in (1, 2, 3):
        remote(
            mod_all.at[peer[k]], mod_all.at[peer[k]], moda_s.at[k], moda_r.at[k], {"tp": peer[k]}
        ).wait_recv()
    for t in range(n_tp):
        cols = slice(t * wid, (t + 1) * wid)
        mod_b[:, cols] = mod_all[t, :, 0:wid]
        mod_a[:, cols] = (1.0 + mod_all[t, :, wid : 2 * wid]) * gain_ref[:, cols]
        mod_g[:, cols] = mod_all[t, :, 2 * wid : 3 * wid]

    def norm_rows(src, mod_row, base, count):
        a_row = mod_a[pl.ds(mod_row, 1), :]
        b_row = mod_b[pl.ds(mod_row, 1), :]

        @pl.loop(0, count // CHUNK, unroll=2)
        def _(c):
            at = pl.multiple_of(c * CHUNK, CHUNK)
            x = src[pl.ds(at, CHUNK), :].astype(F32)
            inv = lax.rsqrt(jnp.mean(x * x, axis=-1, keepdims=True) + EPSILON)
            hbuf[pl.ds(base + at, CHUNK), :] = (x * inv * a_row + b_row).astype(BF16)

    for i in (3, 4, 5):
        loads[i].wait()
    ctx_at = pl.multiple_of(sp * lc, lc)

    @pl.loop(0, samples)
    def _(s):
        norm_rows(ctx_v.at[s], samples, 0, lc)
        ckv[s, pl.ds(ctx_at, lc), :] = jnp.dot(
            hbuf[0:lc, :], wqkv[:, qw : qw + 2 * kw], preferred_element_type=F32
        ).astype(BF16)

    mine = ckv.at[:, pl.ds(ctx_at, lc), :]
    ctx_copies = [
        remote(mine, mine, ctx_s.at[o], ctx_r.at[o], {"sp": sp_peer(o)}) for o in range(1, n_sp)
    ]
    for copy in ctx_copies:
        copy.start()

    for s in (0, 1):
        lat_part(1 + s, s, 0).wait_recv()
        lat_part(1 + s, s, 1).wait_recv()
        lat_copy(3, s, True).start()

    loads[6].wait()
    loads[7].wait()
    lane = lax.broadcasted_iota(jnp.int32, (rows, HEAD_DIM), 1)
    low = lane % (HEAD_DIM // 2) < HEAD_DIM // 4

    def turn(u, cos, sin):
        other = jnp.where(
            low, pltpu.roll(u, HEAD_DIM - HEAD_DIM // 4, 1), pltpu.roll(u, HEAD_DIM // 4, 1)
        )
        return u * cos + other * sin

    halo_up = remote(
        kvbuf.at[:, pl.ds(block, WINDOW), :],
        kvbuf.at[:, pl.ds(0, WINDOW), :],
        halo_s.at[0],
        halo_r.at[0],
        {"sp": sp_peer(1)},
    )
    halo_down = remote(
        kvbuf.at[:, pl.ds(WINDOW, WINDOW), :],
        kvbuf.at[:, pl.ds(WINDOW + block, WINDOW), :],
        halo_s.at[1],
        halo_r.at[1],
        {"sp": sp_peer(n_sp - 1)},
    )

    @pl.loop(0, n_tp)
    def _(k):
        @pl.when(k == 1)
        def _():
            lat_copy(1, 1, False).wait_recv()

        @pl.when(k == 2)
        def _():
            lat_copy(2, 0, False).wait_recv()

        @pl.when(k == 3)
        def _():
            lat_copy(3, 0, True).wait_recv()
            lat_copy(3, 1, True).wait_recv()

        kx, ky = k % 2, k // 2
        bx = tx + kx - 2 * tx * kx
        by = ty + ky - 2 * ty * ky
        b = 2 * by + bx
        for s in range(samples):
            norm_rows(lat_all.at[k, s], s, s * rows, rows)
        at = pl.multiple_of(b * rows, rows)
        cos = cos_ref[pl.ds(at, rows), :]
        sin = sin_ref[pl.ds(at, rows), :]
        for c in range(heads // 2 + 1):
            prod = jnp.dot(
                hbuf[0 : samples * rows, :], wqkv[:, c * 2 * HEAD_DIM : (c + 1) * 2 * HEAD_DIM], preferred_element_type=F32
            )
            for s in range(samples):
                part = prod[s * rows : (s + 1) * rows]
                first = turn(part[:, :HEAD_DIM], cos, sin).astype(BF16)
                if c < heads // 2:
                    second = turn(part[:, HEAD_DIM:], cos, sin).astype(BF16)
                    qbuf[s, b, 2 * c * rows : (2 * c + 1) * rows, :] = first
                    qbuf[s, b, (2 * c + 1) * rows : (2 * c + 2) * rows, :] = second
                else:
                    kvbuf[s, pl.ds(WINDOW + at, rows), 0:HEAD_DIM] = first
                    kvbuf[s, pl.ds(WINDOW + at, rows), HEAD_DIM:] = part[:, HEAD_DIM:].astype(BF16)

        @pl.when(b == 0)
        def _():
            halo_down.start()

        @pl.when(b == n_tp - 1)
        def _():
            halo_up.start()

    loads[8].wait()
    for o in range(1, n_sp):
        got = ckv.at[:, pl.ds(pl.multiple_of(sp_peer(n_sp - o) * lc, lc), lc), :]
        remote(got, got, ctx_s.at[o], ctx_r.at[o], {"sp": sp_peer(o)}).wait_recv()

    scale = HEAD_DIM ** (-0.5) * LOG2E
    seq = block * n_sp
    nums = (((1,), (1,)), ((), ()))

    def rs_copy(i):
        return remote(
            psend.at[i], rs.at[i], rs_s.at[i], rs_r.at[i], {"tp": peer[TARGETS[i]]}
        )

    def pick(i, which):
        value = SENDS[-1][which]
        for j in range(len(SENDS) - 1):
            value = jnp.where(i == j, SENDS[j][which], value)
        return value

    span = 3 * WINDOW
    pair = 2 * rows
    row_id = lax.broadcasted_iota(jnp.int32, (pair, 1), 0)

    @pl.loop(0, 8)
    def _(i):
        k = pick(i, 0)
        s = pick(i, 1)
        kx, ky = k % 2, k // 2
        b = 2 * (ty + ky - 2 * ty * ky) + tx + kx - 2 * tx * kx
        at = pl.multiple_of(b * rows, rows)
        fresh = (i == 0) | (i == 2) | (i == 3) | (i == 6)

        @pl.when(fresh & (b == 0))
        def _():
            halo_up.wait_recv()

        @pl.when(fresh & (b == n_tp - 1))
        def _():
            halo_down.wait_recv()

        kc = ckv[s, :, 0:HEAD_DIM]
        vc = ckv[s, :, HEAD_DIM:]
        kl = kvbuf[s, pl.ds(at, span), 0:HEAD_DIM]
        vl = kvbuf[s, pl.ds(at, span), HEAD_DIM:]
        key = lax.broadcasted_iota(jnp.int32, (pair, span), 1)
        query = lax.broadcasted_iota(jnp.int32, (pair, span), 0) % rows
        pos = key + (sp * block + b * rows - WINDOW)
        allowed = (key >= query) & (key <= query + 2 * WINDOW) & (pos >= 0) & (pos < seq)
        for c in range(heads // 2):
            q = qbuf[s, b, c * pair : (c + 1) * pair, :]
            sc = lax.dot_general(q, kc, nums, preferred_element_type=F32)
            sl = lax.dot_general(q, kl, nums, preferred_element_type=F32)
            sl = jnp.where(allowed, sl, NEGATIVE)
            sink2 = jnp.where(row_id < rows, sink_ref[0, 2 * c], sink_ref[0, 2 * c + 1]) * LOG2E
            top = jnp.maximum(
                jnp.max(sc, axis=-1, keepdims=True), jnp.max(sl, axis=-1, keepdims=True)
            )
            top = jnp.maximum(top * scale, sink2)
            ec = jnp.exp2(sc * scale - top)
            el = jnp.exp2(sl * scale - top)
            total = (
                jnp.sum(ec, axis=-1, keepdims=True)
                + jnp.sum(el, axis=-1, keepdims=True)
                + jnp.exp2(sink2 - top)
            )
            o = jnp.dot(ec.astype(BF16), vc, preferred_element_type=F32)
            o = o + jnp.dot(el.astype(BF16), vl, preferred_element_type=F32)
            o = (o / total).astype(BF16)
            abuf[:, 2 * c * HEAD_DIM : (2 * c + 1) * HEAD_DIM] = o[:rows]
            abuf[:, (2 * c + 1) * HEAD_DIM : (2 * c + 2) * HEAD_DIM] = o[rows:]
        for n in range(n_tp):
            cols = slice(n * wid, (n + 1) * wid)
            psend[i, :, cols] = jnp.dot(
                abuf[...], wo[:, cols], preferred_element_type=F32
            ).astype(BF16)

        for j in range(4):

            @pl.when(i == j)
            def _(j=j):
                rs_copy(j).start()

        for j in (4, 5):

            @pl.when(i == j)
            def _(j=j):
                rs_copy(j - 4).wait_recv()

                @pl.loop(0, rows // CHUNK)
                def _(r):
                    part = pl.ds(pl.multiple_of(r * CHUNK, CHUNK), CHUNK)
                    psend[j, part, :] = (
                        psend[j, part, :].astype(F32) + rs[j - 4, part, :].astype(F32)
                    ).astype(BF16)

                rs_copy(j).start()

    for s in range(2):
        rs_copy(2 + s).wait_recv()
        rs_copy(4 + s).wait_recv()
        g_row = mod_g[s : s + 1, :]

        @pl.loop(0, rows // CHUNK)
        def _(r, s=s, g_row=g_row):
            part = pl.ds(pl.multiple_of(r * CHUNK, CHUNK), CHUNK)
            branch = (
                psend[6 + s, part, :].astype(F32)
                + rs[2 + s, part, :].astype(F32)
                + rs[4 + s, part, :].astype(F32)
            )
            out_ref[s, part, :] = (
                lat_all[0, s, part, :].astype(F32) + g_row * branch
            ).astype(BF16)

    for copy in mod_copies + all_copies + ctx_copies:
        copy.wait_send()
    for k, s in ((1, 1), (2, 0)):
        lat_copy(k, s, False).wait_send()
        lat_part(k, k - 1, 0).wait_send()
        lat_part(k, k - 1, 1).wait_send()
    for s in (0, 1):
        lat_copy(3, s, True).wait_send()
    halo_up.wait_send()
    halo_down.wait_send()
    for i in range(6):
        rs_copy(i).wait_send()


def local(
    n_sp,
    n_tp,
    latent,
    context,
    condition,
    ctx_condition,
    norm_gain,
    w_shift,
    w_scale,
    w_gate,
    w_query,
    w_key,
    w_value,
    w_out,
    sink,
):
    rows, samples, width = latent.shape
    lc = context.shape[0]
    wid = w_shift.shape[1]
    depth = w_shift.shape[0]
    qw, kw = w_query.shape[1], w_key.shape[1]
    heads = qw // HEAD_DIM
    block = rows * n_tp
    assert n_tp == 4 and samples == 2 and kw == HEAD_DIM and rows == WINDOW and block % GRID_W == 0 and heads % 2 == 0
    quarter = HEAD_DIM // 4
    lane = jnp.arange(HEAD_DIM, dtype=jnp.int32)
    freqs = 10000.0 ** (-(lane % quarter).astype(F32) / quarter)
    sign = jnp.where(lane % (2 * quarter) < quarter, -1.0, 1.0).astype(F32)
    grid_rows = block // GRID_W
    first = lax.axis_index("sp") * grid_rows

    def table(position):
        angle = position.astype(F32)[:, None] * freqs[None, :]
        return jnp.stack([jnp.cos(angle), jnp.sin(angle) * sign[None, :]])

    row_table = table(first + jnp.arange(grid_rows, dtype=jnp.int32))
    col_table = table(jnp.arange(GRID_W, dtype=jnp.int32))
    hbm = pl.BlockSpec(memory_space=pl.ANY)
    vmem = pl.BlockSpec(memory_space=pltpu.VMEM)
    smem = pl.BlockSpec(memory_space=pltpu.SMEM)
    dma = pltpu.SemaphoreType.DMA
    mixed = pl.pallas_call(
        functools.partial(kernel, n_sp),
        out_shape=jax.ShapeDtypeStruct((samples, rows, width), BF16),
        in_specs=[hbm, hbm, vmem, vmem, vmem, hbm, hbm, hbm, hbm, hbm, hbm, hbm, smem, vmem, vmem],
        out_specs=vmem,
        scratch_shapes=[
            pltpu.VMEM((n_tp, samples, rows, width), BF16),
            pltpu.VMEM((samples, lc, width), BF16),
            pltpu.VMEM((3, depth, wid), BF16),
            pltpu.VMEM((width, qw + 2 * kw), BF16),
            pltpu.VMEM((qw, width), BF16),
            pltpu.VMEM((8, depth), F32),
            pltpu.VMEM((n_sp, 8, 3 * wid), F32),
            pltpu.VMEM((n_tp, 8, 3 * wid), F32),
            pltpu.VMEM((8, width), F32),
            pltpu.VMEM((8, width), F32),
            pltpu.VMEM((8, width), F32),
            pltpu.VMEM((max(samples * rows, lc), width), BF16),
            pltpu.VMEM((samples, n_tp, heads * rows, HEAD_DIM), BF16),
            pltpu.VMEM((samples, block + 2 * WINDOW, 2 * kw), BF16),
            pltpu.VMEM((samples, lc * n_sp, 2 * kw), BF16),
            pltpu.VMEM((rows, qw), BF16),
            pltpu.VMEM((block, HEAD_DIM), F32),
            pltpu.VMEM((block, HEAD_DIM), F32),
            pltpu.VMEM((8, rows, width), BF16),
            pltpu.VMEM((6, rows, width), BF16),
            dma((9,)),
            dma((n_sp,)),
            dma((n_sp,)),
            dma((n_tp,)),
            dma((n_tp,)),
            dma((n_tp, 2)),
            dma((n_tp, 2)),
            dma((n_tp, 2)),
            dma((n_tp, 2)),
            dma((n_sp,)),
            dma((n_sp,)),
            dma((2,)),
            dma((2,)),
            dma((6,)),
            dma((6,)),
        ],
        compiler_params=pltpu.CompilerParams(
            collective_id=0, has_side_effects=True, vmem_limit_bytes=60 * 1024 * 1024
        ),
        name="step",
    )(
        latent.transpose(1, 0, 2),
        context.transpose(1, 0, 2),
        condition,
        ctx_condition,
        norm_gain[None],
        w_shift,
        w_scale,
        w_gate,
        w_query,
        w_key,
        w_value,
        w_out,
        sink[None],
        row_table,
        col_table,
    )
    return mixed.transpose(1, 0, 2)


def solution(mesh):
    return jax.shard_map(
        functools.partial(local, mesh.shape["sp"], mesh.shape["tp"]),
        mesh=mesh,
        in_specs=(
            P(("sp", "tp"), "dp", None),
            P("sp", "dp", None),
            P("dp", "sp"),
            P("sp"),
            P(),
            P("sp", "tp"),
            P("sp", "tp"),
            P("sp", "tp"),
            P(None, "tp"),
            P(None, "tp"),
            P(None, "tp"),
            P("tp", None),
            P("tp"),
        ),
        out_specs=P(("sp", "tp"), "dp", None),
        check_vma=False,
    )
```

```python
import functools
import math

import jax
import jax.numpy as jnp
from jax import lax
from jax.experimental import pallas as pl
from jax.experimental.pallas import tpu as pltpu
from jax.sharding import PartitionSpec as P

HEAD_DIM = 128
WINDOW = 128
GRID_W = 64
EPSILON = 1e-06
NEGATIVE = -1e30
MESH = pl.DeviceIdType.MESH
F32 = jnp.float32
BF16 = jnp.bfloat16
LOG2E = math.log2(math.e)
CHUNK = 16
SENDS = ((3, 0), (3, 1), (1, 0), (2, 1), (2, 0), (1, 1), (0, 0), (0, 1))
TARGETS = (1, 2, 1, 2, 2, 1)


def kernel(
    n_sp,
    lat_hbm,
    ctx_hbm,
    cond_ref,
    cctx_ref,
    gain_ref,
    wsh_hbm,
    wsc_hbm,
    wga_hbm,
    wq_hbm,
    wk_hbm,
    wv_hbm,
    wo_hbm,
    sink_ref,
    row_cos,
    row_sin,
    col_cos,
    col_sin,
    out_ref,
    lat_all,
    ctx_v,
    wmod,
    wqkv,
    wo,
    act_s,
    mod_p,
    mod_all,
    mod_a,
    mod_b,
    mod_g,
    hbuf,
    qbuf,
    kvbuf,
    ckv,
    abuf,
    cos_ref,
    sin_ref,
    psend,
    rs,

    loc_sem,
    modp_s,
    modp_r,
    moda_s,
    moda_r,
    lat_s,
    lat_r,
    early_s,
    early_r,
    ctx_s,
    ctx_r,
    halo_s,
    halo_r,
    rs_s,
    rs_r,
):
    samples, rows, width = lat_hbm.shape
    n_tp = mod_all.shape[0]
    wid = wmod.shape[2]
    qw = wq_hbm.shape[1]
    kw = wk_hbm.shape[1]
    heads = qw // HEAD_DIM
    lc = ctx_hbm.shape[1]
    block = rows * n_tp
    sp = lax.axis_index("sp")
    tp = lax.axis_index("tp")
    tx, ty = tp % 2, tp // 2
    peer = {1: 2 * ty + 1 - tx, 2: 2 * (1 - ty) + tx, 3: 3 - tp}

    def sp_peer(o):
        return lax.rem(sp + o, n_sp)

    loads = [
        pltpu.make_async_copy(wsh_hbm, wmod.at[0], loc_sem.at[0]),
        pltpu.make_async_copy(wsc_hbm, wmod.at[1], loc_sem.at[1]),
        pltpu.make_async_copy(wga_hbm, wmod.at[2], loc_sem.at[2]),
        pltpu.make_async_copy(ctx_hbm, ctx_v, loc_sem.at[3]),
        pltpu.make_async_copy(wk_hbm, wqkv.at[:, pl.ds(qw, kw)], loc_sem.at[4]),
        pltpu.make_async_copy(wv_hbm, wqkv.at[:, pl.ds(qw + kw, kw)], loc_sem.at[5]),
        pltpu.make_async_copy(lat_hbm, lat_all.at[0], loc_sem.at[6]),
        pltpu.make_async_copy(wq_hbm, wqkv.at[:, pl.ds(0, qw)], loc_sem.at[7]),
        pltpu.make_async_copy(wo_hbm, wo, loc_sem.at[8]),
    ]
    for load in loads:
        load.start()

    barrier = pltpu.get_barrier_semaphore()
    for o in range(1, n_sp):
        pl.semaphore_signal(barrier, inc=1, device_id={"sp": sp_peer(o)}, device_id_type=MESH)
    for k in (1, 2, 3):
        pl.semaphore_signal(barrier, inc=1, device_id={"tp": peer[k]}, device_id_type=MESH)
    pl.semaphore_wait(barrier, n_sp - 1 + n_tp - 1)

    def remote(src, dst, ssem, rsem, dev):
        return pltpu.make_async_remote_copy(
            src_ref=src, dst_ref=dst, send_sem=ssem, recv_sem=rsem, device_id=dev, device_id_type=MESH
        )

    act_s[...] = jnp.zeros_like(act_s)
    cv = cond_ref[...].astype(F32)
    act_s[0:samples, :] = cv / (1.0 + jnp.exp(-cv))
    cc = cctx_ref[...].astype(F32).reshape(1, -1)
    act_s[samples : samples + 1, :] = cc / (1.0 + jnp.exp(-cc))
    both = act_s[...].astype(BF16)
    for m in range(3):
        loads[m].wait()
        mod_p[0, :, m * wid : (m + 1) * wid] = jnp.dot(both, wmod[m], preferred_element_type=F32)
    mod_copies = [
        remote(mod_p.at[0], mod_p.at[o], modp_s.at[o], modp_r.at[o], {"sp": sp_peer(o)})
        for o in range(1, n_sp)
    ]
    for copy in mod_copies:
        copy.start()

    def lat_copy(k, s, relay):
        if not relay:
            return remote(
                lat_hbm.at[s], lat_all.at[k, s], lat_s.at[k, s], lat_r.at[k, s], {"tp": peer[k]}
            )
        via, to = (1, 2) if s == 0 else (2, 1)
        return remote(
            lat_all.at[via, s], lat_all.at[3, s], lat_s.at[3, s], lat_r.at[3, s], {"tp": peer[to]}
        )

    half = rows // 2

    def lat_part(k, s, p):
        part = pl.ds(p * half, half)
        return remote(
            lat_hbm.at[s, part], lat_all.at[k, s, part], early_s.at[k, p], early_r.at[k, p], {"tp": peer[k]}
        )

    lat_part(1, 0, 0).start()
    lat_part(2, 1, 0).start()

    for by_row, by_col, table in ((row_cos, col_cos, cos_ref), (row_sin, col_sin, sin_ref)):
        left = lax.broadcasted_iota(jnp.int32, (GRID_W, HEAD_DIM), 1) < HEAD_DIM // 2
        for r in range(block // GRID_W):
            table[r * GRID_W : (r + 1) * GRID_W, :] = jnp.where(
                left, by_row[r : r + 1, :], by_col[...]
            )

    for copy in mod_copies:
        copy.wait_recv()
    total = mod_p[0]
    for o in range(1, n_sp):
        total = total + mod_p[o]
    mod_all[tp] = total
    all_copies = [
        remote(mod_all.at[tp], mod_all.at[tp], moda_s.at[k], moda_r.at[k], {"tp": peer[k]})
        for k in (1, 2, 3)
    ]
    for copy in all_copies:
        copy.start()
    lat_part(1, 0, 1).start()
    lat_part(2, 1, 1).start()
    lat_copy(1, 1, False).start()
    lat_copy(2, 0, False).start()
    for k in (1, 2, 3):
        remote(
            mod_all.at[peer[k]], mod_all.at[peer[k]], moda_s.at[k], moda_r.at[k], {"tp": peer[k]}
        ).wait_recv()
    for t in range(n_tp):
        cols = slice(t * wid, (t + 1) * wid)
        mod_b[:, cols] = mod_all[t, :, 0:wid]
        mod_a[:, cols] = (1.0 + mod_all[t, :, wid : 2 * wid]) * gain_ref[:, cols]
        mod_g[:, cols] = mod_all[t, :, 2 * wid : 3 * wid]

    def norm_rows(src, mod_row, base, count):
        a_row = mod_a[pl.ds(mod_row, 1), :]
        b_row = mod_b[pl.ds(mod_row, 1), :]

        @pl.loop(0, count // CHUNK, unroll=4)
        def _(c):
            at = pl.multiple_of(c * CHUNK, CHUNK)
            x = src[pl.ds(at, CHUNK), :].astype(F32)
            inv = lax.rsqrt(jnp.mean(x * x, axis=-1, keepdims=True) + EPSILON)
            hbuf[pl.ds(base + at, CHUNK), :] = (x * inv * a_row + b_row).astype(BF16)

    for i in (3, 4, 5):
        loads[i].wait()
    ctx_at = pl.multiple_of(sp * lc, lc)

    @pl.loop(0, samples)
    def _(s):
        norm_rows(ctx_v.at[s], samples, 0, lc)
        ckv[s, pl.ds(ctx_at, lc), :] = jnp.dot(
            hbuf[0:lc, :], wqkv[:, qw : qw + 2 * kw], preferred_element_type=F32
        ).astype(BF16)

    mine = ckv.at[:, pl.ds(ctx_at, lc), :]
    ctx_copies = [
        remote(mine, mine, ctx_s.at[o], ctx_r.at[o], {"sp": sp_peer(o)}) for o in range(1, n_sp)
    ]
    for copy in ctx_copies:
        copy.start()

    for s in (0, 1):
        lat_part(1 + s, s, 0).wait_recv()
        lat_part(1 + s, s, 1).wait_recv()
        lat_copy(3, s, True).start()

    loads[6].wait()
    loads[7].wait()
    lane = lax.broadcasted_iota(jnp.int32, (rows, HEAD_DIM), 1)
    low = lane % (HEAD_DIM // 2) < HEAD_DIM // 4

    def turn(u, cos, sin):
        other = jnp.where(
            low, pltpu.roll(u, HEAD_DIM - HEAD_DIM // 4, 1), pltpu.roll(u, HEAD_DIM // 4, 1)
        )
        return u * cos + other * sin

    halo_up = remote(
        kvbuf.at[:, pl.ds(block, WINDOW), :],
        kvbuf.at[:, pl.ds(0, WINDOW), :],
        halo_s.at[0],
        halo_r.at[0],
        {"sp": sp_peer(1)},
    )
    halo_down = remote(
        kvbuf.at[:, pl.ds(WINDOW, WINDOW), :],
        kvbuf.at[:, pl.ds(WINDOW + block, WINDOW), :],
        halo_s.at[1],
        halo_r.at[1],
        {"sp": sp_peer(n_sp - 1)},
    )

    @pl.loop(0, n_tp)
    def _(k):
        @pl.when(k == 1)
        def _():
            lat_copy(1, 1, False).wait_recv()

        @pl.when(k == 2)
        def _():
            lat_copy(2, 0, False).wait_recv()

        @pl.when(k == 3)
        def _():
            lat_copy(3, 0, True).wait_recv()
            lat_copy(3, 1, True).wait_recv()

        kx, ky = k % 2, k // 2
        bx = tx + kx - 2 * tx * kx
        by = ty + ky - 2 * ty * ky
        b = 2 * by + bx
        for s in range(samples):
            norm_rows(lat_all.at[k, s], s, s * rows, rows)
        at = pl.multiple_of(b * rows, rows)
        cos = cos_ref[pl.ds(at, rows), :]
        sin = sin_ref[pl.ds(at, rows), :]
        for c in range(heads // 2 + 1):
            prod = jnp.dot(
                hbuf[0 : samples * rows, :], wqkv[:, c * 2 * HEAD_DIM : (c + 1) * 2 * HEAD_DIM], preferred_element_type=F32
            )
            for s in range(samples):
                part = prod[s * rows : (s + 1) * rows]
                first = turn(part[:, :HEAD_DIM], cos, sin).astype(BF16)
                if c < heads // 2:
                    second = turn(part[:, HEAD_DIM:], cos, sin).astype(BF16)
                    qbuf[s, b, 2 * c * rows : (2 * c + 1) * rows, :] = first
                    qbuf[s, b, (2 * c + 1) * rows : (2 * c + 2) * rows, :] = second
                else:
                    kvbuf[s, pl.ds(WINDOW + at, rows), 0:HEAD_DIM] = first
                    kvbuf[s, pl.ds(WINDOW + at, rows), HEAD_DIM:] = part[:, HEAD_DIM:].astype(BF16)

        @pl.when(b == 0)
        def _():
            halo_down.start()

        @pl.when(b == n_tp - 1)
        def _():
            halo_up.start()

    loads[8].wait()
    for o in range(1, n_sp):
        got = ckv.at[:, pl.ds(pl.multiple_of(sp_peer(n_sp - o) * lc, lc), lc), :]
        remote(got, got, ctx_s.at[o], ctx_r.at[o], {"sp": sp_peer(o)}).wait_recv()

    scale = HEAD_DIM ** (-0.5) * LOG2E
    seq = block * n_sp
    nums = (((1,), (1,)), ((), ()))

    def rs_copy(i):
        return remote(
            psend.at[i], rs.at[i], rs_s.at[i], rs_r.at[i], {"tp": peer[TARGETS[i]]}
        )

    def pick(i, which):
        value = SENDS[-1][which]
        for j in range(len(SENDS) - 1):
            value = jnp.where(i == j, SENDS[j][which], value)
        return value

    span = 3 * WINDOW
    pair = 2 * rows
    row_id = lax.broadcasted_iota(jnp.int32, (pair, 1), 0)

    @pl.loop(0, 8)
    def _(i):
        k = pick(i, 0)
        s = pick(i, 1)
        kx, ky = k % 2, k // 2
        b = 2 * (ty + ky - 2 * ty * ky) + tx + kx - 2 * tx * kx
        at = pl.multiple_of(b * rows, rows)
        fresh = (i == 0) | (i == 2) | (i == 3) | (i == 6)

        @pl.when(fresh & (b == 0))
        def _():
            halo_up.wait_recv()

        @pl.when(fresh & (b == n_tp - 1))
        def _():
            halo_down.wait_recv()

        kc = ckv[s, :, 0:HEAD_DIM]
        vc = ckv[s, :, HEAD_DIM:]
        kl = kvbuf[s, pl.ds(at, span), 0:HEAD_DIM]
        vl = kvbuf[s, pl.ds(at, span), HEAD_DIM:]
        key = lax.broadcasted_iota(jnp.int32, (pair, span), 1)
        query = lax.broadcasted_iota(jnp.int32, (pair, span), 0) % rows
        pos = key + (sp * block + b * rows - WINDOW)
        allowed = (key >= query) & (key <= query + 2 * WINDOW) & (pos >= 0) & (pos < seq)
        for c in range(heads // 2):
            q = qbuf[s, b, c * pair : (c + 1) * pair, :]
            sc = lax.dot_general(q, kc, nums, preferred_element_type=F32)
            sl = lax.dot_general(q, kl, nums, preferred_element_type=F32)
            sl = jnp.where(allowed, sl, NEGATIVE)
            sink2 = jnp.where(row_id < rows, sink_ref[0, 2 * c], sink_ref[0, 2 * c + 1]) * LOG2E
            top = jnp.maximum(
                jnp.max(sc, axis=-1, keepdims=True), jnp.max(sl, axis=-1, keepdims=True)
            )
            top = jnp.maximum(top * scale, sink2)
            ec = jnp.exp2(sc * scale - top)
            el = jnp.exp2(sl * scale - top)
            total = (
                jnp.sum(ec, axis=-1, keepdims=True)
                + jnp.sum(el, axis=-1, keepdims=True)
                + jnp.exp2(sink2 - top)
            )
            o = jnp.dot(ec.astype(BF16), vc, preferred_element_type=F32)
            o = o + jnp.dot(el.astype(BF16), vl, preferred_element_type=F32)
            o = (o / total).astype(BF16)
            abuf[:, 2 * c * HEAD_DIM : (2 * c + 1) * HEAD_DIM] = o[:rows]
            abuf[:, (2 * c + 1) * HEAD_DIM : (2 * c + 2) * HEAD_DIM] = o[rows:]
        for n in range(n_tp):
            cols = slice(n * wid, (n + 1) * wid)
            psend[i, :, cols] = jnp.dot(
                abuf[...], wo[:, cols], preferred_element_type=F32
            ).astype(BF16)

        for j in range(4):

            @pl.when(i == j)
            def _(j=j):
                rs_copy(j).start()

        for j in (4, 5):

            @pl.when(i == j)
            def _(j=j):
                rs_copy(j - 4).wait_recv()

                @pl.loop(0, rows // CHUNK)
                def _(r):
                    part = pl.ds(pl.multiple_of(r * CHUNK, CHUNK), CHUNK)
                    psend[j, part, :] = (
                        psend[j, part, :].astype(F32) + rs[j - 4, part, :].astype(F32)
                    ).astype(BF16)

                rs_copy(j).start()

    for s in range(2):
        rs_copy(2 + s).wait_recv()
        rs_copy(4 + s).wait_recv()
        g_row = mod_g[s : s + 1, :]

        @pl.loop(0, rows // CHUNK, unroll=2)
        def _(r, s=s, g_row=g_row):
            part = pl.ds(pl.multiple_of(r * CHUNK, CHUNK), CHUNK)
            branch = (
                psend[6 + s, part, :].astype(F32)
                + rs[2 + s, part, :].astype(F32)
                + rs[4 + s, part, :].astype(F32)
            )
            out_ref[s, part, :] = (
                lat_all[0, s, part, :].astype(F32) + g_row * branch
            ).astype(BF16)

    for copy in mod_copies + all_copies + ctx_copies:
        copy.wait_send()
    for k, s in ((1, 1), (2, 0)):
        lat_copy(k, s, False).wait_send()
        lat_part(k, k - 1, 0).wait_send()
        lat_part(k, k - 1, 1).wait_send()
    for s in (0, 1):
        lat_copy(3, s, True).wait_send()
    halo_up.wait_send()
    halo_down.wait_send()
    for i in range(6):
        rs_copy(i).wait_send()


def local(
    n_sp,
    n_tp,
    latent,
    context,
    condition,
    ctx_condition,
    norm_gain,
    w_shift,
    w_scale,
    w_gate,
    w_query,
    w_key,
    w_value,
    w_out,
    sink,
):
    rows, samples, width = latent.shape
    lc = context.shape[0]
    wid = w_shift.shape[1]
    depth = w_shift.shape[0]
    qw, kw = w_query.shape[1], w_key.shape[1]
    heads = qw // HEAD_DIM
    block = rows * n_tp
    assert n_tp == 4 and samples == 2 and kw == HEAD_DIM and rows == WINDOW and block % GRID_W == 0 and heads % 2 == 0
    quarter = HEAD_DIM // 4
    lane = jnp.arange(HEAD_DIM, dtype=jnp.int32)
    freqs = 10000.0 ** (-(lane % quarter).astype(F32) / quarter)
    sign = jnp.where(lane % (2 * quarter) < quarter, -1.0, 1.0).astype(F32)
    grid_rows = block // GRID_W
    first = lax.axis_index("sp") * grid_rows

    def table(position):
        angle = position.astype(F32)[:, None] * freqs[None, :]
        return jnp.cos(angle), jnp.sin(angle) * sign[None, :]

    row_table = table(first + jnp.arange(grid_rows, dtype=jnp.int32))
    col_table = table(jnp.arange(GRID_W, dtype=jnp.int32))
    hbm = pl.BlockSpec(memory_space=pl.ANY)
    vmem = pl.BlockSpec(memory_space=pltpu.VMEM)
    smem = pl.BlockSpec(memory_space=pltpu.SMEM)
    dma = pltpu.SemaphoreType.DMA
    mixed = pl.pallas_call(
        functools.partial(kernel, n_sp),
        out_shape=jax.ShapeDtypeStruct((samples, rows, width), BF16),
        in_specs=[hbm, hbm, vmem, vmem, vmem, hbm, hbm, hbm, hbm, hbm, hbm, hbm, smem, vmem, vmem, vmem, vmem],
        out_specs=vmem,
        scratch_shapes=[
            pltpu.VMEM((n_tp, samples, rows, width), BF16),
            pltpu.VMEM((samples, lc, width), BF16),
            pltpu.VMEM((3, depth, wid), BF16),
            pltpu.VMEM((width, qw + 2 * kw), BF16),
            pltpu.VMEM((qw, width), BF16),
            pltpu.VMEM((8, depth), F32),
            pltpu.VMEM((n_sp, 8, 3 * wid), F32),
            pltpu.VMEM((n_tp, 8, 3 * wid), F32),
            pltpu.VMEM((8, width), F32),
            pltpu.VMEM((8, width), F32),
            pltpu.VMEM((8, width), F32),
            pltpu.VMEM((max(samples * rows, lc), width), BF16),
            pltpu.VMEM((samples, n_tp, heads * rows, HEAD_DIM), BF16),
            pltpu.VMEM((samples, block + 2 * WINDOW, 2 * kw), BF16),
            pltpu.VMEM((samples, lc * n_sp, 2 * kw), BF16),
            pltpu.VMEM((rows, qw), BF16),
            pltpu.VMEM((block, HEAD_DIM), F32),
            pltpu.VMEM((block, HEAD_DIM), F32),
            pltpu.VMEM((8, rows, width), BF16),
            pltpu.VMEM((6, rows, width), BF16),
            dma((9,)),
            dma((n_sp,)),
            dma((n_sp,)),
            dma((n_tp,)),
            dma((n_tp,)),
            dma((n_tp, 2)),
            dma((n_tp, 2)),
            dma((n_tp, 2)),
            dma((n_tp, 2)),
            dma((n_sp,)),
            dma((n_sp,)),
            dma((2,)),
            dma((2,)),
            dma((6,)),
            dma((6,)),
        ],
        compiler_params=pltpu.CompilerParams(
            collective_id=0, has_side_effects=True, vmem_limit_bytes=60 * 1024 * 1024
        ),
        name="step",
    )(
        latent.transpose(1, 0, 2),
        context.transpose(1, 0, 2),
        condition,
        ctx_condition,
        norm_gain[None],
        w_shift,
        w_scale,
        w_gate,
        w_query,
        w_key,
        w_value,
        w_out,
        sink[None],
        *row_table,
        *col_table,
    )
    return mixed.transpose(1, 0, 2)


def solution(mesh):
    return jax.shard_map(
        functools.partial(local, mesh.shape["sp"], mesh.shape["tp"]),
        mesh=mesh,
        in_specs=(
            P(("sp", "tp"), "dp", None),
            P("sp", "dp", None),
            P("dp", "sp"),
            P("sp"),
            P(),
            P("sp", "tp"),
            P("sp", "tp"),
            P("sp", "tp"),
            P(None, "tp"),
            P(None, "tp"),
            P(None, "tp"),
            P("tp", None),
            P("tp"),
        ),
        out_specs=P(("sp", "tp"), "dp", None),
        check_vma=False,
    )
```
